32 devices in a mesh: sp: 8 (over z, y), tp: 4 (over x, core).
Axes of the slice: x: 2, y: 2, z: 4, core: 2. Of those that a mesh axis runs over, the one named last changes fastest.
Arguments:
- inputs: bfloat16 [4096, 4096], P(('sp', 'tp')), may hold values from -42 to 42
- a_query_w: bfloat16 [4096, 2048], P(None, 'tp'), may hold values from -0.12570312 to 0.12570312
- a_key_w: bfloat16 [4096, 2048], P(None, 'tp'), may hold values from -0.12570312 to 0.12570312
- a_value_w: bfloat16 [4096, 2048], P(None, 'tp'), may hold values from -0.09375 to 0.09375
- b_query_w: bfloat16 [4096, 2048], P(None, 'tp'), may hold values from -0.12570312 to 0.12570312
- b_key_w: bfloat16 [4096, 512], P(None, 'tp'), may hold values from -0.12570312 to 0.12570312
- b_value_w: bfloat16 [4096, 512], P(None, 'tp'), may hold values from -0.09375 to 0.09375
- head_lambda: float32 [16], P('tp'), may hold values from 0.3 to 0.8
- head_gain: float32 [128], replicated, may hold values from 0.1 to 1.9
- sink_logit: float32 [32], P('tp'), may hold values from 2 to 7
- a_out_w: bfloat16 [2048, 4096], P('tp'), may hold values from -0.125 to 0.125
- b_out_w: bfloat16 [2048, 4096], P('tp'), may hold values from -0.625 to 0.625
Outputs:
- mixed: bfloat16 [4096, 4096], P(('sp', 'tp'))
The draws below stay inside these ranges and needn't reach their ends.
All inputs are finite; a program needn't handle non-finite values.
Results may differ from the reference program's by a relative error of at most 0.015.
Values may be sent and summed in bfloat16 or wider, within the bound.
A program may use at most 128 MiB of HBM per device.

```python
import math
import jax
import jax.numpy as jnp
from jax import lax

D = 4096
A_HEADS = 16
B_HEADS = 32
KV_HEADS = 8
HEAD_DIM = 64
VALUE_DIM = 128
WINDOW = 128
TOKENS = 4096
N_TP = 4


def plain_noise(key, salt, columns):
    values = jnp.clip(jax.random.normal(jax.random.fold_in(key, salt), (D, columns), jnp.float32), -6.0, 6.0)
    return values * (1.32 * D ** (-0.5))


def draw_inputs(key, part):
    values = jnp.clip(jax.random.normal(jax.random.fold_in(key, 10), (TOKENS, D), jnp.float32), -6.0, 6.0)
    return values.astype(jnp.bfloat16)


def draw_a_query_w(key, part):
    columns = 2 * A_HEADS * HEAD_DIM
    values = plain_noise(key, 11, columns)
    return values.astype(jnp.bfloat16)


def draw_a_key_w(key, part):
    columns = 2 * A_HEADS * HEAD_DIM
    values = plain_noise(key, 12, columns)
    return values.astype(jnp.bfloat16)


def draw_b_query_w(key, part):
    columns = B_HEADS * HEAD_DIM
    values = plain_noise(key, 13, columns)
    return values.astype(jnp.bfloat16)


def draw_b_key_w(key, part):
    columns = KV_HEADS * HEAD_DIM
    values = plain_noise(key, 14, columns)
    return values.astype(jnp.bfloat16)


def block_levels(key, shape, shards, smallest, high):
    gain, own = 1.0, jax.random.fold_in(key, 6)
    for axis_at, shards_of in shards:
        steps = jnp.exp(jax.random.uniform(jax.random.fold_in(own, axis_at), (shards_of,), jnp.float32, smallest / len(shards), high / len(shards)))
        gain = gain * jnp.repeat(steps, shape[axis_at] // shards_of).reshape([-1 if axis == axis_at else 1 for axis in range(len(shape))])
    return gain


def normal_values(own_key, extent, width, reach, cuts=(), kind=jnp.bfloat16):
    level = block_levels(own_key, extent, cuts, -0.22, 0.18) if cuts else 1.0
    drawn = jax.random.normal(own_key, extent, jnp.float32) * width * level
    return jnp.minimum(jnp.maximum(drawn, -reach), reach).astype(kind)


def setup_inputs(seed: int = 0) -> dict:
    seeds = jax.random.split(jax.random.key(seed), 13)
    inputs = draw_inputs(jax.random.fold_in(seeds[12], 71), 0)
    a_query_w = draw_a_query_w(jax.random.fold_in(seeds[12], 71), 0)
    a_key_w = draw_a_key_w(jax.random.fold_in(seeds[12], 71), 0)
    a_value_w = normal_values(seeds[3], (D, A_HEADS * VALUE_DIM), D ** -0.5, 0.09375, ((1, 4),))
    b_query_w = draw_b_query_w(jax.random.fold_in(seeds[12], 71), 0)
    b_key_w = draw_b_key_w(jax.random.fold_in(seeds[12], 71), 0)
    b_value_w = normal_values(seeds[6], (D, KV_HEADS * HEAD_DIM), D ** -0.5, 0.09375, ((1, 4),))
    head_lambda = jnp.clip(0.3 + 0.5 * jax.random.uniform(seeds[7], (A_HEADS,), jnp.float32) ** block_levels(seeds[7], (A_HEADS,), ((0, 4),), -0.2, 0.2), 0.3, 0.8)
    head_gain = jnp.clip(1.0 + 0.18 * jax.random.normal(seeds[8], (VALUE_DIM,), jnp.float32), 0.1, 1.9)
    sink_logit = jnp.clip(2.0 + 5.0 * jax.random.uniform(seeds[9], (B_HEADS,), jnp.float32) ** block_levels(seeds[9], (B_HEADS,), ((0, 4),), -0.2, 0.2), 2.0, 7.0)
    a_out_w = normal_values(seeds[10], (A_HEADS * VALUE_DIM, D), (A_HEADS * VALUE_DIM) ** -0.5, 0.125, ((0, 4),))
    b_out_w = normal_values(seeds[11], (B_HEADS * HEAD_DIM, D), (5.0 * (B_HEADS * HEAD_DIM) ** -0.5), 0.625, ((0, 4),))
    return {"inputs": inputs, "a_query_w": a_query_w, "a_key_w": a_key_w, "a_value_w": a_value_w, "b_query_w": b_query_w, "b_key_w": b_key_w, "b_value_w": b_value_w, "head_lambda": head_lambda, "head_gain": head_gain, "sink_logit": sink_logit, "a_out_w": a_out_w, "b_out_w": b_out_w}


norm_eps = 0.0001
head_scale = 0.8
mask_fill = -1e+30

def rounded(value):
    return lax.optimization_barrier(value.astype(jnp.bfloat16)).astype(jnp.float32)

def reference(inputs, a_query_w, a_key_w, a_value_w, b_query_w, b_key_w, b_value_w, head_lambda, head_gain, sink_logit, a_out_w, b_out_w):
    length = inputs.shape[0]
    group_size = B_HEADS // KV_HEADS
    score_scale = HEAD_DIM ** (-0.5)
    a_query = jnp.dot(inputs, a_query_w, preferred_element_type=jnp.float32).astype(jnp.bfloat16).reshape(length, A_HEADS, 2, HEAD_DIM)
    a_key = jnp.dot(inputs, a_key_w, preferred_element_type=jnp.float32).astype(jnp.bfloat16).reshape(length, A_HEADS, 2, HEAD_DIM)
    a_value = jnp.dot(inputs, a_value_w, preferred_element_type=jnp.float32).astype(jnp.bfloat16).reshape(length, A_HEADS, VALUE_DIM)
    b_query = jnp.dot(inputs, b_query_w, preferred_element_type=jnp.float32).astype(jnp.bfloat16).reshape(length, KV_HEADS, group_size, HEAD_DIM)
    b_key = jnp.dot(inputs, b_key_w, preferred_element_type=jnp.float32).astype(jnp.bfloat16).reshape(length, KV_HEADS, HEAD_DIM)
    b_value = jnp.dot(inputs, b_value_w, preferred_element_type=jnp.float32).astype(jnp.bfloat16).reshape(length, KV_HEADS, HEAD_DIM)
    query_span = math.gcd(length, 128)
    span_count = length // query_span
    key_pos = jnp.arange(length, dtype=jnp.int32)
    keys_wide = a_key.astype(jnp.float32)
    values_wide = a_value.astype(jnp.float32)

    def differential(block_index):
        block_start = block_index * query_span
        queries = lax.dynamic_slice_in_dim(a_query, block_start, query_span, 0).astype(jnp.float32)
        scores = jnp.einsum('qhmd,khmd->hmqk', queries, keys_wide) * score_scale
        query_pos = block_start + jnp.arange(query_span, dtype=jnp.int32)
        allowed = query_pos[:, None] >= key_pos[None, :]
        scores = jnp.where(allowed, scores, mask_fill)
        row_top = lax.optimization_barrier(jnp.max(scores, axis=-1, keepdims=True))
        weights = jnp.where(allowed, jnp.exp(scores - row_top), 0.0)
        row_total = lax.optimization_barrier(jnp.sum(weights, axis=-1))
        means = jnp.einsum('hmqk,khe->hmqe', rounded(weights), values_wide) / row_total[..., None]
        difference = means[:, 0] - head_lambda[:, None, None] * means[:, 1]
        mean_square = lax.optimization_barrier(jnp.mean(difference * difference, axis=-1, keepdims=True))
        return (difference * lax.rsqrt(mean_square + norm_eps) * head_gain * head_scale).astype(jnp.bfloat16)
    a_heads = lax.map(differential, jnp.arange(span_count, dtype=jnp.int32))
    a_heads = jnp.transpose(a_heads, (1, 0, 2, 3)).reshape(A_HEADS, length, VALUE_DIM)
    pad_keys = jnp.concatenate([jnp.zeros((WINDOW, KV_HEADS, HEAD_DIM), jnp.bfloat16), b_key], axis=0).astype(jnp.float32)
    pad_values = jnp.concatenate([jnp.zeros((WINDOW, KV_HEADS, HEAD_DIM), jnp.bfloat16), b_value], axis=0).astype(jnp.float32)
    sink_term = sink_logit.reshape(KV_HEADS, group_size)[:, :, None]

    def windowed(block_index):
        block_start = block_index * query_span
        queries = lax.dynamic_slice_in_dim(b_query, block_start, query_span, 0).astype(jnp.float32)
        block_keys = lax.dynamic_slice_in_dim(pad_keys, block_start, query_span + WINDOW, 0)
        block_values = lax.dynamic_slice_in_dim(pad_values, block_start, query_span + WINDOW, 0)
        scores = jnp.einsum('qhgd,khd->hgqk', queries, block_keys) * score_scale
        query_pos = block_start + jnp.arange(query_span, dtype=jnp.int32)
        near_pos = block_start - WINDOW + jnp.arange(query_span + WINDOW, dtype=jnp.int32)
        distance = query_pos[:, None] - near_pos[None, :]
        allowed = (distance >= 0) & (distance < WINDOW) & (near_pos[None, :] >= 0)
        scores = jnp.where(allowed, scores, mask_fill)
        row_top = jnp.maximum(lax.optimization_barrier(jnp.max(scores, axis=-1)), sink_term)
        weights = jnp.where(allowed, jnp.exp(scores - row_top[..., None]), 0.0)
        row_total = lax.optimization_barrier(jnp.sum(weights, axis=-1)) + jnp.exp(sink_term - row_top)
        probs = weights / row_total[..., None]
        block_out = jnp.einsum('hgqk,khd->qhgd', rounded(probs), block_values)
        return block_out.reshape(query_span, B_HEADS * HEAD_DIM).astype(jnp.bfloat16)
    b_heads = lax.map(windowed, jnp.arange(span_count, dtype=jnp.int32)).reshape(length, B_HEADS * HEAD_DIM)
    heads_local = A_HEADS // N_TP
    cols_local = B_HEADS * HEAD_DIM // N_TP
    summed = jnp.zeros((length, D), jnp.float32)
    for group_index in range(N_TP):
        a_part = a_heads[group_index * heads_local:(group_index + 1) * heads_local].astype(jnp.float32)
        a_weight = a_out_w[group_index * heads_local * VALUE_DIM:(group_index + 1) * heads_local * VALUE_DIM]
        a_weight = a_weight.reshape(heads_local, VALUE_DIM, D).astype(jnp.float32)
        b_part = b_heads[:, group_index * cols_local:(group_index + 1) * cols_local]
        b_weight = b_out_w[group_index * cols_local:(group_index + 1) * cols_local]
        partial_sum = jnp.einsum('hqe,hen->qn', a_part, a_weight) + jnp.dot(b_part, b_weight, preferred_element_type=jnp.float32)
        summed = summed + rounded(partial_sum)
    return summed.astype(jnp.bfloat16)
```

```python
import functools

import jax
import jax.numpy as jnp
from jax import lax
from jax.experimental import pallas as pl
from jax.experimental.pallas import tpu as pltpu
from jax.sharding import PartitionSpec as P

HEAD_DIM = 64
VALUE_DIM = 128
WINDOW = 128
norm_eps = 0.0001
head_scale = 0.8
mask_fill = -1e30
MESH = pl.DeviceIdType.MESH
F32 = jnp.float32
BF16 = jnp.bfloat16


def mm(a, b):
    return jnp.dot(a, b, preferred_element_type=F32)


def mm_t(a, b):
    return lax.dot_general(a, b, (((1,), (1,)), ((), ())), preferred_element_type=F32)


def attend_kernel(
    n, n_tp, n_split,
    lam, sink, aq, ak, av, bq, bk, bv, gain, wa_hbm, wb_hbm,
    out,
    kbuf, vbuf, qbuf, kext, vext, hbuf, obuf, qs, m_s, l_s, acc_s, b_heads,
    wa, wb, dsend, dbuf, own, xsend, xbuf,
    send_sem, recv_sem, ret_send, ret_recv, near_send, near_recv, w_sem,
    d_send, d_recv, x_send, x_recv,
):
    me = lax.axis_index("sp")
    t = lax.axis_index("tp")
    rows = aq.shape[0]
    sub = rows // n_split
    pair = jnp.where(lax.rem(t, 2) == 0, t + 1, t - 1)
    core = lax.rem(t, 2)
    chip = t // 2
    chips = n_tp // 2
    n_chunks = wa.shape[0]
    width = wa.shape[2]
    part = rows // n_tp

    barrier = pltpu.get_barrier_semaphore()
    for o in range(1, n):
        pl.semaphore_signal(barrier, inc=1, device_id={"sp": lax.rem(me + o, n)}, device_id_type=MESH)
    for o in range(1, n_tp):
        pl.semaphore_signal(barrier, inc=1, device_id={"tp": lax.rem(t + o, n_tp)}, device_id_type=MESH)
    pl.semaphore_wait(barrier, n - 1 + n_tp - 1)

    def subblock(source, j):
        return jnp.where(lax.rem(source, 2) == 0, j, n_split - 1 - j)

    def pieces(d):
        h = d // n_split
        start = pl.multiple_of(subblock(me, lax.rem(d, n_split)) * sub, sub)
        cols = pl.ds(pl.multiple_of(h * VALUE_DIM, VALUE_DIM), VALUE_DIM)
        return (
            (aq.at[pl.ds(start, sub), cols], qbuf),
            (ak.at[:, cols], kbuf),
            (av.at[:, cols], vbuf),
        )

    def near_copies():
        return [
            pltpu.make_async_remote_copy(
                src_ref=src.at[pl.ds(rows - WINDOW, WINDOW)],
                dst_ref=dst.at[pl.ds(0, WINDOW)],
                send_sem=near_send.at[c],
                recv_sem=near_recv.at[c],
                device_id={"sp": lax.rem(me + 1, n)},
                device_id_type=MESH,
            )
            for c, (src, dst) in enumerate(((bk, kext), (bv, vext)))
        ]

    @pl.when(me < n - 1)
    def _():
        for copy in near_copies():
            copy.start()

    def send_copies(o):
        d = lax.rem(me + o, n)
        return [
            pltpu.make_async_remote_copy(
                src_ref=src,
                dst_ref=dst.at[me],
                send_sem=send_sem.at[o, c],
                recv_sem=recv_sem.at[me, c],
                device_id={"sp": d},
                device_id_type=MESH,
            )
            for c, (src, dst) in enumerate(pieces(d))
        ]

    def local_copies():
        return [
            pltpu.make_async_copy(src, dst.at[me], recv_sem.at[me, c])
            for c, (src, dst) in enumerate(pieces(me))
        ]

    for copy in local_copies():
        copy.start()

    @pl.loop(1, n)
    def _(o):
        for copy in send_copies(o):
            copy.start()

    def weight_copies(cc):
        at = pl.ds(pl.multiple_of(cc * width, width), width)
        return (
            pltpu.make_async_copy(wa_hbm.at[:, at], wa.at[cc], w_sem.at[cc, 0]),
            pltpu.make_async_copy(wb_hbm.at[:, at], wb.at[cc], w_sem.at[cc, 1]),
        )

    @pl.loop(0, n_chunks)
    def _(cc):
        for copy in weight_copies(cc):
            copy.start()

    kext[pl.ds(WINDOW, rows)] = bk[...]
    vext[pl.ds(WINDOW, rows)] = bv[...]

    @pl.when(me == 0)
    def _():
        kext[pl.ds(0, WINDOW)] = jnp.zeros((WINDOW, kext.shape[1]), BF16)
        vext[pl.ds(0, WINDOW)] = jnp.zeros((WINDOW, vext.shape[1]), BF16)

    @pl.when(me > 0)
    def _():
        for copy in near_copies():
            copy.wait_recv()

    kv_heads = bk.shape[1] // HEAD_DIM
    group = bq.shape[1] // bk.shape[1]
    q_iota = lax.broadcasted_iota(jnp.int32, (WINDOW, 2 * WINDOW), 0)
    k_iota = lax.broadcasted_iota(jnp.int32, (WINDOW, 2 * WINDOW), 1)

    @pl.loop(0, rows // WINDOW)
    def _(b):
        base = pl.multiple_of(b * WINDOW, WINDOW)
        first = (b == 0) & (me == 0)
        distance = q_iota + WINDOW - k_iota
        low = jnp.where(first, WINDOW, 0)
        allowed = (distance >= 0) & (distance < WINDOW) & (k_iota >= low)
        queries = bq[pl.ds(base, WINDOW), :].astype(F32) * HEAD_DIM ** (-0.5)
        queries = queries.astype(BF16)
        keys = kext[pl.ds(base, 2 * WINDOW), :]
        values = vext[pl.ds(base, 2 * WINDOW), :]
        for g in range(kv_heads):
            key = keys[:, g * HEAD_DIM : (g + 1) * HEAD_DIM]
            value = values[:, g * HEAD_DIM : (g + 1) * HEAD_DIM]
            for two in range(group // 2):
                both = []
                for e in range(2):
                    h = g * group + two * 2 + e
                    s = mm_t(queries[:, h * HEAD_DIM : (h + 1) * HEAD_DIM], key)
                    s = jnp.where(allowed, s, mask_fill)
                    top = jnp.maximum(jnp.max(s, axis=-1, keepdims=True), sink[h])
                    p = jnp.exp(s - top)
                    total = jnp.sum(p, axis=-1, keepdims=True) + jnp.exp(sink[h] - top)
                    both.append(mm((p * (1.0 / total)).astype(BF16), value).astype(BF16))
                at = (g * group + two * 2) * HEAD_DIM
                b_heads[pl.ds(base, WINDOW), at : at + 2 * HEAD_DIM] = jnp.concatenate(both, axis=1)

    my_head = me // n_split
    my_part = lax.rem(me, n_split)
    lane = lax.broadcasted_iota(jnp.int32, (sub, VALUE_DIM), 1)

    def ret_copy(i):
        row = pl.ds(pl.multiple_of(subblock(i, my_part) * sub, sub), sub)
        return pltpu.make_async_remote_copy(
            src_ref=obuf.at[i],
            dst_ref=hbuf.at[my_head, row],
            send_sem=ret_send.at[i],
            recv_sem=ret_recv.at[me],
            device_id={"sp": i},
            device_id_type=MESH,
        )

    def ret_local(i):
        row = pl.ds(pl.multiple_of(subblock(i, my_part) * sub, sub), sub)
        return pltpu.make_async_copy(obuf.at[i], hbuf.at[my_head, row], ret_recv.at[me])

    @pl.loop(0, n)
    def _(i):
        for c, (buf) in enumerate((qbuf, kbuf, vbuf)):
            pltpu.make_async_copy(buf.at[i], buf.at[i], recv_sem.at[i, c]).wait()
        q = qbuf[i].astype(F32) * HEAD_DIM ** (-0.5)
        qs[0] = jnp.where(lane < HEAD_DIM, q, 0.0).astype(BF16)
        qs[1] = jnp.where(lane >= HEAD_DIM, q, 0.0).astype(BF16)
        m_s[...] = jnp.full(m_s.shape, mask_fill, F32)
        l_s[...] = jnp.zeros(l_s.shape, F32)
        acc_s[...] = jnp.zeros(acc_s.shape, F32)
        first_row = subblock(i, my_part) * sub

        def block(j, diagonal):
            k = kbuf[j]
            v = vbuf[j]
            for m in range(2):
                s = mm_t(qs[m], k)
                if diagonal:
                    qpos = first_row + lax.broadcasted_iota(jnp.int32, s.shape, 0)
                    s = jnp.where(lax.broadcasted_iota(jnp.int32, s.shape, 1) <= qpos, s, mask_fill)
                old = m_s[m]
                new = jnp.maximum(old, jnp.max(s, axis=-1, keepdims=True))
                shrink = jnp.exp(old - new)
                p = jnp.exp(s - new[:, :1])
                folded = p[:, :VALUE_DIM]
                for c in range(1, s.shape[1] // VALUE_DIM):
                    folded = folded + p[:, c * VALUE_DIM : (c + 1) * VALUE_DIM]
                m_s[m] = new
                l_s[m] = l_s[m] * shrink + folded
                acc_s[m] = acc_s[m] * shrink + mm(p.astype(BF16), v)

        @pl.loop(0, i)
        def _(j):
            block(j, False)

        block(i, True)
        mean = [acc_s[m] / jnp.sum(l_s[m], axis=-1, keepdims=True) for m in range(2)]
        diff = mean[0] - lam[my_head] * mean[1]
        square = jnp.mean(diff * diff, axis=-1, keepdims=True)
        obuf[i] = (diff * lax.rsqrt(square + norm_eps) * gain[...] * head_scale).astype(BF16)

        @pl.when(i == me)
        def _():
            ret_local(i).start()

        @pl.when(i != me)
        def _():
            ret_copy(i).start()

    @pl.loop(0, n)
    def _(d):
        row = pl.ds(pl.multiple_of(subblock(me, lax.rem(d, n_split)) * sub, sub), sub)
        place = hbuf.at[d // n_split, row]
        pltpu.make_async_copy(place, place, ret_recv.at[d]).wait()

    local_heads = hbuf.shape[0]

    def project(row, cc):
        total = mm(b_heads[pl.ds(row, part), :], wb[cc])
        for h in range(local_heads):
            total = total + mm(hbuf[h, pl.ds(row, part), :], wa[cc, h * VALUE_DIM : (h + 1) * VALUE_DIM, :])
        return total

    def row_of(x, c):
        return pl.multiple_of((2 * x + c) * part, part)

    def d_copy(cc):
        return pltpu.make_async_remote_copy(
            src_ref=dsend.at[cc], dst_ref=dbuf.at[cc],
            send_sem=d_send.at[cc], recv_sem=d_recv.at[cc],
            device_id={"tp": pair}, device_id_type=MESH,
        )

    def x_copy(cc, o):
        to = lax.rem(chip + o, chips)
        return pltpu.make_async_remote_copy(
            src_ref=xsend.at[cc, o - 1], dst_ref=xbuf.at[cc, o - 1],
            send_sem=x_send.at[cc, o - 1], recv_sem=x_recv.at[cc, o - 1],
            device_id={"tp": 2 * to + core}, device_id_type=MESH,
        )

    def pass_on(cc):
        d_copy(cc).wait_recv()
        for o in range(1, chips):
            xsend[cc, o - 1] = (own[cc, o] + dbuf[cc, o].astype(F32)).astype(BF16)
            x_copy(cc, o).start()

    @pl.loop(0, n_chunks)
    def _(cc):
        for copy in weight_copies(cc):
            copy.wait()
        for o in range(chips):
            dsend[cc, o] = project(row_of(lax.rem(chip + o, chips), 1 - core), cc).astype(BF16)
        d_copy(cc).start()
        for o in range(chips):
            own[cc, o] = project(row_of(lax.rem(chip + o, chips), core), cc)

        @pl.when(cc > 0)
        def _():
            pass_on(cc - 1)

    pass_on(n_chunks - 1)

    @pl.loop(0, n_chunks)
    def _(cc):
        total = own[cc, 0] + dbuf[cc, 0].astype(F32)
        for o in range(1, chips):
            x_copy(cc, o).wait_recv()
            total = total + xbuf[cc, o - 1].astype(F32)
        out[:, pl.ds(pl.multiple_of(cc * width, width), width)] = total.astype(BF16)

    @pl.when(me < n - 1)
    def _():
        for copy in near_copies():
            copy.wait_send()

    @pl.loop(1, n)
    def _(o):
        for copy in send_copies(o):
            copy.wait_send()

    @pl.loop(0, n)
    def _(i):
        @pl.when(i != me)
        def _():
            ret_copy(i).wait_send()

    @pl.loop(0, n_chunks)
    def _(cc):
        d_copy(cc).wait_send()
        for o in range(1, chips):
            x_copy(cc, o).wait_send()


def attend(n, n_tp, lam, sink, aq, ak, av, bq, bk, bv, gain, wa, wb):
    rows = aq.shape[0]
    local_heads = lam.shape[0]
    n_split = n // local_heads
    sub = rows // n_split
    model = wa.shape[1]
    width = 512
    n_chunks = model // width
    chips = n_tp // 2
    part = rows // n_tp
    vm = pl.BlockSpec(memory_space=pltpu.VMEM)
    sm = pl.BlockSpec(memory_space=pltpu.SMEM)
    hbm = pl.BlockSpec(memory_space=pl.ANY)
    dma = pltpu.SemaphoreType.DMA
    return pl.pallas_call(
        functools.partial(attend_kernel, n, n_tp, n_split),
        out_shape=jax.ShapeDtypeStruct((part, model), BF16),
        in_specs=[sm, sm, vm, vm, vm, vm, vm, vm, vm, hbm, hbm],
        out_specs=vm,
        scratch_shapes=[
            pltpu.VMEM((n, rows, VALUE_DIM), BF16),
            pltpu.VMEM((n, rows, VALUE_DIM), BF16),
            pltpu.VMEM((n, sub, VALUE_DIM), BF16),
            pltpu.VMEM((WINDOW + rows, bk.shape[1]), BF16),
            pltpu.VMEM((WINDOW + rows, bv.shape[1]), BF16),
            pltpu.VMEM((local_heads, rows, VALUE_DIM), BF16),
            pltpu.VMEM((n, sub, VALUE_DIM), BF16),
            pltpu.VMEM((2, sub, VALUE_DIM), BF16),
            pltpu.VMEM((2, sub, VALUE_DIM), F32),
            pltpu.VMEM((2, sub, VALUE_DIM), F32),
            pltpu.VMEM((2, sub, VALUE_DIM), F32),
            pltpu.VMEM(bq.shape, BF16),
            pltpu.VMEM((n_chunks, wa.shape[0], width), BF16),
            pltpu.VMEM((n_chunks, wb.shape[0], width), BF16),
            pltpu.VMEM((n_chunks, chips, part, width), BF16),
            pltpu.VMEM((n_chunks, chips, part, width), BF16),
            pltpu.VMEM((n_chunks, chips, part, width), F32),
            pltpu.VMEM((n_chunks, chips - 1, part, width), BF16),
            pltpu.VMEM((n_chunks, chips - 1, part, width), BF16),
            dma((n, 3)),
            dma((n, 3)),
            dma((n,)),
            dma((n,)),
            dma((2,)),
            dma((2,)),
            dma((n_chunks, 2)),
            dma((n_chunks,)),
            dma((n_chunks,)),
            dma((n_chunks, chips - 1)),
            dma((n_chunks, chips - 1)),
        ],
        compiler_params=pltpu.CompilerParams(
            collective_id=0, has_side_effects=True, vmem_limit_bytes=62 * 1024 * 1024
        ),
    )(lam, sink, aq, ak, av, bq, bk, bv, gain, wa, wb)


def solution(mesh):
    n, n_tp = mesh.shape["sp"], mesh.shape["tp"]

    def shards(
        inputs, a_query_w, a_key_w, a_value_w, b_query_w, b_key_w, b_value_w,
        head_lambda, head_gain, sink_logit, a_out_w, b_out_w,
    ):
        gathered = lax.all_gather(inputs, "tp", axis=0, tiled=True)
        projected = [
            mm(gathered, matrix).astype(BF16)
            for matrix in (a_query_w, a_key_w, a_value_w, b_query_w, b_key_w, b_value_w)
        ]
        return attend(
            n, n_tp, head_lambda, sink_logit, *projected, head_gain.reshape(1, VALUE_DIM), a_out_w, b_out_w
        )

    return jax.shard_map(
        shards,
        mesh=mesh,
        in_specs=(
            P(("sp", "tp"), None),
            P(None, "tp"),
            P(None, "tp"),
            P(None, "tp"),
            P(None, "tp"),
            P(None, "tp"),
            P(None, "tp"),
            P("tp"),
            P(),
            P("tp"),
            P("tp", None),
            P("tp", None),
        ),
        out_specs=P(("sp", "tp"), None),
        check_vma=False,
    )
```

```python
import functools

import jax
import jax.numpy as jnp
from jax import lax
from jax.experimental import pallas as pl
from jax.experimental.pallas import tpu as pltpu
from jax.sharding import PartitionSpec as P

HEAD_DIM = 64
VALUE_DIM = 128
WINDOW = 128
norm_eps = 0.0001
head_scale = 0.8
mask_fill = -1e30
MESH = pl.DeviceIdType.MESH
F32 = jnp.float32
BF16 = jnp.bfloat16


def mm(a, b):
    return jnp.dot(a, b, preferred_element_type=F32)


def mm_t(a, b):
    return lax.dot_general(a, b, (((1,), (1,)), ((), ())), preferred_element_type=F32)


def attend_kernel(
    n, n_tp, n_split,
    lam, sink, gain, x_hbm, wq_hbm, wk_hbm, wv_hbm, bwq_hbm, bwk_hbm, bwv_hbm, wa_hbm, wb_hbm,
    out,
    xown, xrem, wq, wk, wv, bwq, bwk, bwv, aq, akv, bq,
    kv, qbuf, kext, vext, hbuf, obuf, qs, m_s, l_s, acc_s, b_heads,
    wa, wb, dsend, dbuf, own, xsend, xbuf,
    x_sem, p_sem, g_send, g_recv, f_send, f_recv, own_send, own_recv,
    kv_send, kv_recv, q_send, q_recv, ret_send, ret_recv, near_send, near_recv, w_sem,
    d_send, d_recv, x_send, x_recv,
):
    me = lax.axis_index("sp")
    t = lax.axis_index("tp")
    rows = aq.shape[0]
    sub = rows // n_split
    pair = jnp.where(lax.rem(t, 2) == 0, t + 1, t - 1)
    core = lax.rem(t, 2)
    chip = t // 2
    chips = n_tp // 2
    n_chunks = wa.shape[0]
    width = wa.shape[2]
    part = rows // n_tp
    half = part // 2
    model = x_hbm.shape[1]

    x_copy_in = pltpu.make_async_copy(x_hbm, xown.at[core], x_sem)
    x_copy_in.start()
    weights = ((wk_hbm, wk), (wv_hbm, wv), (wq_hbm, wq), (bwk_hbm, bwk), (bwv_hbm, bwv), (bwq_hbm, bwq))
    p_copies = [pltpu.make_async_copy(src, dst, p_sem.at[c]) for c, (src, dst) in enumerate(weights)]
    for copy in p_copies:
        copy.start()

    barrier = pltpu.get_barrier_semaphore()
    for o in range(1, n):
        pl.semaphore_signal(barrier, inc=1, device_id={"sp": lax.rem(me + o, n)}, device_id_type=MESH)
    for o in range(1, n_tp):
        pl.semaphore_signal(barrier, inc=1, device_id={"tp": lax.rem(t + o, n_tp)}, device_id_type=MESH)
    pl.semaphore_wait(barrier, n - 1 + n_tp - 1)
    x_copy_in.wait()

    def g_copy(o, hf):
        return pltpu.make_async_remote_copy(
            src_ref=xown.at[core, pl.ds(hf * half, half)], dst_ref=xrem.at[o - 1, hf, core],
            send_sem=g_send.at[o - 1, hf], recv_sem=g_recv.at[o - 1, hf],
            device_id={"tp": 2 * lax.rem(chip + o, chips) + core}, device_id_type=MESH,
        )

    def f_copy(o, hf, c):
        return pltpu.make_async_remote_copy(
            src_ref=xrem.at[o - 1, hf, c], dst_ref=xrem.at[o - 1, hf, c],
            send_sem=f_send.at[o - 1, hf], recv_sem=f_recv.at[o - 1, hf],
            device_id={"tp": pair}, device_id_type=MESH,
        )

    def own_copy(c):
        return pltpu.make_async_remote_copy(
            src_ref=xown.at[c], dst_ref=xown.at[c], send_sem=own_send, recv_sem=own_recv,
            device_id={"tp": pair}, device_id_type=MESH,
        )

    for hf in range(2):
        for o in range(1, chips):
            g_copy(o, hf).start()
    own_copy(core).start()

    def weight_copies(cc):
        at = pl.ds(pl.multiple_of(cc * width, width), width)
        return (
            pltpu.make_async_copy(wa_hbm.at[:, at], wa.at[cc], w_sem.at[cc, 0]),
            pltpu.make_async_copy(wb_hbm.at[:, at], wb.at[cc], w_sem.at[cc, 1]),
        )

    def column_steps(w):
        step = min(w.shape[1], 256)
        return [(at, step) for at in range(0, w.shape[1], step)]

    def project_rows(load, put, first=None):
        for c, (_, w) in enumerate(weights):
            if first is not None:
                @pl.when(first)
                def _():
                    p_copies[c].wait()
            for at, step in column_steps(w):
                put(c, at, step, mm(load(), w[:, at : at + step]).astype(BF16))

    def put_rows(c, at, step, row, value):
        count = value.shape[0]
        if c == 2:
            aq[pl.ds(row, count), at : at + step] = value
        elif c == 3:
            kext[pl.ds(row + WINDOW, count), at : at + step] = value
        elif c == 4:
            vext[pl.ds(row + WINDOW, count), at : at + step] = value
        else:
            bq[pl.ds(row, count), at : at + step] = value

    def subblock(source, j):
        return jnp.where(lax.rem(source, 2) == 0, j, n_split - 1 - j)

    def head_columns(d):
        return pl.ds(pl.multiple_of(d // n_split * VALUE_DIM, VALUE_DIM), VALUE_DIM)

    def send_kv(x, hf):
        for kind in range(2):
            for o in range(n):
                d = lax.rem(me + o, n)
                if hf is None:
                    src = akv.at[kind, x, :, :, :, head_columns(d)]
                    dst = kv.at[me, kind, x]
                else:
                    src = akv.at[kind, x, :, hf, :, head_columns(d)]
                    dst = kv.at[me, kind, x, :, hf]
                if o == 0:
                    pltpu.make_async_copy(src, dst, kv_recv.at[me]).start()
                else:
                    pltpu.make_async_remote_copy(
                        src_ref=src, dst_ref=dst, send_sem=kv_send.at[o], recv_sem=kv_recv.at[me],
                        device_id={"sp": d}, device_id_type=MESH,
                    ).start()

    def q_piece(d):
        start = pl.multiple_of(subblock(me, lax.rem(d, n_split)) * sub, sub)
        return aq.at[pl.ds(start, sub), head_columns(d)]

    def q_copy(o):
        d = lax.rem(me + o, n)
        return pltpu.make_async_remote_copy(
            src_ref=q_piece(d), dst_ref=qbuf.at[me], send_sem=q_send.at[o], recv_sem=q_recv.at[me],
            device_id={"sp": d}, device_id_type=MESH,
        )

    def near_copies():
        return [
            pltpu.make_async_remote_copy(
                src_ref=buf.at[pl.ds(rows, WINDOW)],
                dst_ref=buf.at[pl.ds(0, WINDOW)],
                send_sem=near_send.at[c],
                recv_sem=near_recv.at[c],
                device_id={"sp": lax.rem(me + 1, n)},
                device_id_type=MESH,
            )
            for c, buf in enumerate((kext, vext))
        ]

    @pl.loop(0, 2)
    def _(step):
        c_of = jnp.where(step == 0, core, 1 - core)
        row = pl.multiple_of((2 * chip + c_of) * part, part)

        @pl.when(step == 1)
        def _():
            own_copy(1 - core).wait_recv()

        def put(c, at, w, value):
            if c < 2:
                akv[c, chip, c_of, :, :, at : at + w] = value.reshape(2, half, w)
            else:
                put_rows(c, at, w, row, value)

        project_rows(lambda: xown[c_of], put, first=step == 0)

    send_kv(chip, None)

    for o in range(1, chips):
        x = lax.rem(chip + chips - o, chips)

        @pl.loop(0, 2)
        def _(hf):
            g_copy(o, hf).wait_recv()
            f_copy(o, hf, core).start()
            f_copy(o, hf, 1 - core).wait_recv()

            def put(c, at, w, value):
                value = value.reshape(2, half, w)
                for k in range(2):
                    if c < 2:
                        akv[c, x, k, hf, :, at : at + w] = value[k]
                    else:
                        row = pl.multiple_of((2 * x + k) * part + hf * half, half)
                        put_rows(c, at, w, row, value[k])

            project_rows(lambda: xrem[o - 1, hf].reshape(part, model), put)

            if o == chips - 1:
                @pl.when((hf == 1) & (me < n - 1))
                def _():
                    for copy in near_copies():
                        copy.start()

            send_kv(x, hf)

    pltpu.make_async_copy(q_piece(me), qbuf.at[me], q_recv.at[me]).start()
    for o in range(1, n):
        q_copy(o).start()

    @pl.loop(0, n_chunks)
    def _(cc):
        for copy in weight_copies(cc):
            copy.start()

    @pl.when(me == 0)
    def _():
        kext[pl.ds(0, WINDOW)] = jnp.zeros((WINDOW, kext.shape[1]), BF16)
        vext[pl.ds(0, WINDOW)] = jnp.zeros((WINDOW, vext.shape[1]), BF16)

    kv_heads = kext.shape[1] // HEAD_DIM
    group = bq.shape[1] // kext.shape[1]
    blocks = rows // WINDOW
    q_iota = lax.broadcasted_iota(jnp.int32, (WINDOW, 2 * WINDOW), 0)
    k_iota = lax.broadcasted_iota(jnp.int32, (WINDOW, 2 * WINDOW), 1)

    @pl.loop(0, blocks)
    def _(step):
        b = lax.rem(step + 1, blocks)

        @pl.when((b == 0) & (me > 0))
        def _():
            for copy in near_copies():
                copy.wait_recv()

        base = pl.multiple_of(b * WINDOW, WINDOW)
        first = (b == 0) & (me == 0)
        distance = q_iota + WINDOW - k_iota
        low = jnp.where(first, WINDOW, 0)
        allowed = (distance >= 0) & (distance < WINDOW) & (k_iota >= low)
        queries = bq[pl.ds(base, WINDOW), :].astype(F32) * HEAD_DIM ** (-0.5)
        queries = queries.astype(BF16)
        keys = kext[pl.ds(base, 2 * WINDOW), :]
        values = vext[pl.ds(base, 2 * WINDOW), :]
        for g in range(kv_heads):
            key = keys[:, g * HEAD_DIM : (g + 1) * HEAD_DIM]
            value = values[:, g * HEAD_DIM : (g + 1) * HEAD_DIM]
            for two in range(group // 2):
                both = []
                for e in range(2):
                    h = g * group + two * 2 + e
                    s = mm_t(queries[:, h * HEAD_DIM : (h + 1) * HEAD_DIM], key)
                    s = jnp.where(allowed, s, mask_fill)
                    top = jnp.maximum(jnp.max(s, axis=-1, keepdims=True), sink[h])
                    p = jnp.exp(s - top)
                    total = jnp.sum(p, axis=-1, keepdims=True) + jnp.exp(sink[h] - top)
                    both.append(mm((p * (1.0 / total)).astype(BF16), value).astype(BF16))
                at = (g * group + two * 2) * HEAD_DIM
                b_heads[pl.ds(base, WINDOW), at : at + 2 * HEAD_DIM] = jnp.concatenate(both, axis=1)

    my_head = me // n_split
    my_part = lax.rem(me, n_split)
    lane = lax.broadcasted_iota(jnp.int32, (sub, VALUE_DIM), 1)

    def ret_copy(i):
        row = pl.ds(pl.multiple_of(subblock(i, my_part) * sub, sub), sub)
        return pltpu.make_async_remote_copy(
            src_ref=obuf.at[i],
            dst_ref=hbuf.at[my_head, row],
            send_sem=ret_send.at[i],
            recv_sem=ret_recv.at[me],
            device_id={"sp": i},
            device_id_type=MESH,
        )

    def ret_local(i):
        row = pl.ds(pl.multiple_of(subblock(i, my_part) * sub, sub), sub)
        return pltpu.make_async_copy(obuf.at[i], hbuf.at[my_head, row], ret_recv.at[me])

    @pl.loop(0, n)
    def _(i):
        pltpu.make_async_copy(kv.at[i], kv.at[i], kv_recv.at[i]).wait()
        pltpu.make_async_copy(qbuf.at[i], qbuf.at[i], q_recv.at[i]).wait()
        q = qbuf[i].astype(F32) * HEAD_DIM ** (-0.5)
        qs[0] = jnp.where(lane < HEAD_DIM, q, 0.0).astype(BF16)
        qs[1] = jnp.where(lane >= HEAD_DIM, q, 0.0).astype(BF16)
        m_s[...] = jnp.full(m_s.shape, mask_fill, F32)
        l_s[...] = jnp.zeros(l_s.shape, F32)
        acc_s[...] = jnp.zeros(acc_s.shape, F32)
        first_row = subblock(i, my_part) * sub

        def block(j, diagonal):
            k = kv[j, 0].reshape(rows, VALUE_DIM)
            v = kv[j, 1].reshape(rows, VALUE_DIM)
            for m in range(2):
                s = mm_t(qs[m], k)
                if diagonal:
                    qpos = first_row + lax.broadcasted_iota(jnp.int32, s.shape, 0)
                    s = jnp.where(lax.broadcasted_iota(jnp.int32, s.shape, 1) <= qpos, s, mask_fill)
                old = m_s[m]
                new = jnp.maximum(old, jnp.max(s, axis=-1, keepdims=True))
                shrink = jnp.exp(old - new)
                p = jnp.exp(s - new[:, :1])
                folded = p[:, :VALUE_DIM]
                for c in range(1, s.shape[1] // VALUE_DIM):
                    folded = folded + p[:, c * VALUE_DIM : (c + 1) * VALUE_DIM]
                m_s[m] = new
                l_s[m] = l_s[m] * shrink + folded
                acc_s[m] = acc_s[m] * shrink + mm(p.astype(BF16), v)

        @pl.loop(0, i)
        def _(j):
            block(j, False)

        block(i, True)
        mean = [acc_s[m] / jnp.sum(l_s[m], axis=-1, keepdims=True) for m in range(2)]
        diff = mean[0] - lam[my_head] * mean[1]
        square = jnp.mean(diff * diff, axis=-1, keepdims=True)
        obuf[i] = (diff * lax.rsqrt(square + norm_eps) * gain[...] * head_scale).astype(BF16)

        @pl.when(i == me)
        def _():
            ret_local(i).start()

        @pl.when(i != me)
        def _():
            ret_copy(i).start()

    @pl.loop(0, n)
    def _(d):
        row = pl.ds(pl.multiple_of(subblock(me, lax.rem(d, n_split)) * sub, sub), sub)
        place = hbuf.at[d // n_split, row]
        pltpu.make_async_copy(place, place, ret_recv.at[d]).wait()

    local_heads = hbuf.shape[0]

    def project(row, cc):
        total = mm(b_heads[pl.ds(row, part), :], wb[cc])
        for h in range(local_heads):
            total = total + mm(hbuf[h, pl.ds(row, part), :], wa[cc, h * VALUE_DIM : (h + 1) * VALUE_DIM, :])
        return total

    def row_of(x, c):
        return pl.multiple_of((2 * x + c) * part, part)

    def d_copy(cc):
        return pltpu.make_async_remote_copy(
            src_ref=dsend.at[cc], dst_ref=dbuf.at[cc],
            send_sem=d_send.at[cc], recv_sem=d_recv.at[cc],
            device_id={"tp": pair}, device_id_type=MESH,
        )

    def x_copy(cc, o):
        to = lax.rem(chip + o, chips)
        return pltpu.make_async_remote_copy(
            src_ref=xsend.at[cc, o - 1], dst_ref=xbuf.at[cc, o - 1],
            send_sem=x_send.at[cc, o - 1], recv_sem=x_recv.at[cc, o - 1],
            device_id={"tp": 2 * to + core}, device_id_type=MESH,
        )

    def pass_on(cc):
        d_copy(cc).wait_recv()
        for o in range(1, chips):
            xsend[cc, o - 1] = (own[cc, o] + dbuf[cc, o].astype(F32)).astype(BF16)
            x_copy(cc, o).start()

    @pl.loop(0, n_chunks)
    def _(cc):
        for copy in weight_copies(cc):
            copy.wait()
        for o in range(chips):
            dsend[cc, o] = project(row_of(lax.rem(chip + o, chips), 1 - core), cc).astype(BF16)
        d_copy(cc).start()
        for o in range(chips):
            own[cc, o] = project(row_of(lax.rem(chip + o, chips), core), cc)

        @pl.when(cc > 0)
        def _():
            pass_on(cc - 1)

    pass_on(n_chunks - 1)

    @pl.loop(0, n_chunks)
    def _(cc):
        total = own[cc, 0] + dbuf[cc, 0].astype(F32)
        for o in range(1, chips):
            x_copy(cc, o).wait_recv()
            total = total + xbuf[cc, o - 1].astype(F32)
        out[:, pl.ds(pl.multiple_of(cc * width, width), width)] = total.astype(BF16)

    @pl.when(me < n - 1)
    def _():
        for copy in near_copies():
            copy.wait_send()

    @pl.loop(1, n)
    def _(o):
        pltpu.make_async_copy(kv.at[0], kv.at[0], kv_send.at[o]).wait()
        q_copy(o).wait_send()

    own_copy(core).wait_send()
    for o in range(1, chips):
        for hf in range(2):
            g_copy(o, hf).wait_send()
            f_copy(o, hf, core).wait_send()

    @pl.loop(0, n)
    def _(i):
        @pl.when(i != me)
        def _():
            ret_copy(i).wait_send()

    @pl.loop(0, n_chunks)
    def _(cc):
        d_copy(cc).wait_send()
        for o in range(1, chips):
            x_copy(cc, o).wait_send()


def attend(n, n_tp, lam, sink, gain, inputs, wq, wk, wv, bwq, bwk, bwv, wa, wb):
    part, model = inputs.shape
    rows = part * n_tp
    half = part // 2
    local_heads = lam.shape[0]
    n_split = n // local_heads
    sub = rows // n_split
    width = 512
    n_chunks = model // width
    chips = n_tp // 2
    vm = pl.BlockSpec(memory_space=pltpu.VMEM)
    sm = pl.BlockSpec(memory_space=pltpu.SMEM)
    hbm = pl.BlockSpec(memory_space=pl.ANY)
    dma = pltpu.SemaphoreType.DMA
    return pl.pallas_call(
        functools.partial(attend_kernel, n, n_tp, n_split),
        out_shape=jax.ShapeDtypeStruct((part, model), BF16),
        in_specs=[sm, sm, vm] + [hbm] * 9,
        out_specs=vm,
        scratch_shapes=[
            pltpu.VMEM((2, part, model), BF16),
            pltpu.VMEM((chips - 1, 2, 2, half, model), BF16),
            pltpu.VMEM(wq.shape, BF16),
            pltpu.VMEM(wk.shape, BF16),
            pltpu.VMEM(wv.shape, BF16),
            pltpu.VMEM(bwq.shape, BF16),
            pltpu.VMEM(bwk.shape, BF16),
            pltpu.VMEM(bwv.shape, BF16),
            pltpu.VMEM((rows, wq.shape[1]), BF16),
            pltpu.VMEM((2, chips, 2, 2, half, wk.shape[1]), BF16),
            pltpu.VMEM((rows, bwq.shape[1]), BF16),
            pltpu.VMEM((n, 2, chips, 2, 2, half, VALUE_DIM), BF16),
            pltpu.VMEM((n, sub, VALUE_DIM), BF16),
            pltpu.VMEM((WINDOW + rows, bwk.shape[1]), BF16),
            pltpu.VMEM((WINDOW + rows, bwv.shape[1]), BF16),
            pltpu.VMEM((local_heads, rows, VALUE_DIM), BF16),
            pltpu.VMEM((n, sub, VALUE_DIM), BF16),
            pltpu.VMEM((2, sub, VALUE_DIM), BF16),
            pltpu.VMEM((2, sub, VALUE_DIM), F32),
            pltpu.VMEM((2, sub, VALUE_DIM), F32),
            pltpu.VMEM((2, sub, VALUE_DIM), F32),
            pltpu.VMEM((rows, bwq.shape[1]), BF16),
            pltpu.VMEM((n_chunks, wa.shape[0], width), BF16),
            pltpu.VMEM((n_chunks, wb.shape[0], width), BF16),
            pltpu.VMEM((n_chunks, chips, part, width), BF16),
            pltpu.VMEM((n_chunks, chips, part, width), BF16),
            pltpu.VMEM((n_chunks, chips, part, width), F32),
            pltpu.VMEM((n_chunks, chips - 1, part, width), BF16),
            pltpu.VMEM((n_chunks, chips - 1, part, width), BF16),
            dma,
            dma((6,)),
            dma((chips - 1, 2)),
            dma((chips - 1, 2)),
            dma((chips - 1, 2)),
            dma((chips - 1, 2)),
            dma,
            dma,
            dma((n,)),
            dma((n,)),
            dma((n,)),
            dma((n,)),
            dma((n,)),
            dma((n,)),
            dma((2,)),
            dma((2,)),
            dma((n_chunks, 2)),
            dma((n_chunks,)),
            dma((n_chunks,)),
            dma((n_chunks, chips - 1)),
            dma((n_chunks, chips - 1)),
        ],
        compiler_params=pltpu.CompilerParams(
            collective_id=0, has_side_effects=True, vmem_limit_bytes=63 * 1024 * 1024
        ),
    )(lam, sink, gain, inputs, wq, wk, wv, bwq, bwk, bwv, wa, wb)


def solution(mesh):
    n, n_tp = mesh.shape["sp"], mesh.shape["tp"]

    def shards(
        inputs, a_query_w, a_key_w, a_value_w, b_query_w, b_key_w, b_value_w,
        head_lambda, head_gain, sink_logit, a_out_w, b_out_w,
    ):
        return attend(
            n, n_tp, head_lambda, sink_logit, head_gain.reshape(1, VALUE_DIM), inputs,
            a_query_w, a_key_w, a_value_w, b_query_w, b_key_w, b_value_w, a_out_w, b_out_w,
        )

    return jax.shard_map(
        shards,
        mesh=mesh,
        in_specs=(
            P(("sp", "tp"), None),
            P(None, "tp"),
            P(None, "tp"),
            P(None, "tp"),
            P(None, "tp"),
            P(None, "tp"),
            P(None, "tp"),
            P("tp"),
            P(),
            P("tp"),
            P("tp", None),
            P("tp", None),
        ),
        out_specs=P(("sp", "tp"), None),
        check_vma=False,
    )
```

```python
import functools

import jax
import jax.numpy as jnp
from jax import lax
from jax.experimental import pallas as pl
from jax.experimental.pallas import tpu as pltpu
from jax.sharding import PartitionSpec as P

HEAD_DIM = 64
VALUE_DIM = 128
WINDOW = 128
norm_eps = 0.0001
head_scale = 0.8
mask_fill = -1e30
MESH = pl.DeviceIdType.MESH
F32 = jnp.float32
BF16 = jnp.bfloat16


def mm(a, b):
    return jnp.dot(a, b, preferred_element_type=F32)


def mm_t(a, b):
    return lax.dot_general(a, b, (((1,), (1,)), ((), ())), preferred_element_type=F32)


def attend_kernel(
    n, n_tp, n_split,
    lam, sink, gain, x_hbm, wq_hbm, wk_hbm, wv_hbm, bwq_hbm, bwk_hbm, bwv_hbm, wa_hbm, wb_hbm,
    out,
    xown, xrem, wq, wk, wv, bwq, bwk, bwv, aq, akv, bq,
    kv, qbuf, kext, vext, hbuf, obuf, qs, m_s, l_s, acc_s, b_heads,
    wa, wb, dsend, dbuf, own, xsend, xbuf,
    x_sem, p_sem, g_send, g_recv, f_send, f_recv, own_send, own_recv,
    kv_send, kv_recv, q_send, q_recv, ret_send, ret_recv, near_send, near_recv, w_sem,
    d_send, d_recv, x_send, x_recv,
):
    me = lax.axis_index("sp")
    t = lax.axis_index("tp")
    rows = aq.shape[0]
    sub = rows // n_split
    pair = jnp.where(lax.rem(t, 2) == 0, t + 1, t - 1)
    core = lax.rem(t, 2)
    chip = t // 2
    chips = n_tp // 2
    n_chunks = wa.shape[0]
    width = wa.shape[2]
    part = rows // n_tp
    half = part // 2
    model = x_hbm.shape[1]

    x_copy_in = pltpu.make_async_copy(x_hbm, xown.at[core], x_sem)
    x_copy_in.start()
    weights = ((wk_hbm, wk), (wv_hbm, wv), (wq_hbm, wq), (bwk_hbm, bwk), (bwv_hbm, bwv), (bwq_hbm, bwq))
    p_copies = [pltpu.make_async_copy(src, dst, p_sem.at[c]) for c, (src, dst) in enumerate(weights)]
    for copy in p_copies:
        copy.start()

    barrier = pltpu.get_barrier_semaphore()
    for o in range(1, n):
        pl.semaphore_signal(barrier, inc=1, device_id={"sp": lax.rem(me + o, n)}, device_id_type=MESH)
    for o in range(1, n_tp):
        pl.semaphore_signal(barrier, inc=1, device_id={"tp": lax.rem(t + o, n_tp)}, device_id_type=MESH)
    pl.semaphore_wait(barrier, n - 1 + n_tp - 1)
    x_copy_in.wait()

    def g_copy(o, hf):
        return pltpu.make_async_remote_copy(
            src_ref=xown.at[core, pl.ds(hf * half, half)], dst_ref=xrem.at[o - 1, hf, core],
            send_sem=g_send.at[o - 1, hf], recv_sem=g_recv.at[o - 1, hf],
            device_id={"tp": 2 * lax.rem(chip + o, chips) + core}, device_id_type=MESH,
        )

    def f_copy(o, hf, c):
        return pltpu.make_async_remote_copy(
            src_ref=xrem.at[o - 1, hf, c], dst_ref=xrem.at[o - 1, hf, c],
            send_sem=f_send.at[o - 1, hf], recv_sem=f_recv.at[o - 1, hf],
            device_id={"tp": pair}, device_id_type=MESH,
        )

    def own_copy(c):
        return pltpu.make_async_remote_copy(
            src_ref=xown.at[c], dst_ref=xown.at[c], send_sem=own_send, recv_sem=own_recv,
            device_id={"tp": pair}, device_id_type=MESH,
        )

    for hf in range(2):
        for o in range(1, chips):
            g_copy(o, hf).start()
    own_copy(core).start()

    def weight_copies(cc):
        at = pl.ds(pl.multiple_of(cc * width, width), width)
        return (
            pltpu.make_async_copy(wa_hbm.at[:, at], wa.at[cc], w_sem.at[cc, 0]),
            pltpu.make_async_copy(wb_hbm.at[:, at], wb.at[cc], w_sem.at[cc, 1]),
        )

    def column_steps(w):
        step = min(w.shape[1], 256)
        return [(at, step) for at in range(0, w.shape[1], step)]

    def project_rows(load, put, first=None):
        for c, (_, w) in enumerate(weights):
            if first is not None:
                @pl.when(first)
                def _():
                    p_copies[c].wait()
            for at, step in column_steps(w):
                put(c, at, step, mm(load(), w[:, at : at + step]).astype(BF16))

    def put_rows(c, at, step, row, value):
        count = value.shape[0]
        if c == 2:
            aq[pl.ds(row, count), at : at + step] = value
        elif c == 3:
            kext[pl.ds(row + WINDOW, count), at : at + step] = value
        elif c == 4:
            vext[pl.ds(row + WINDOW, count), at : at + step] = value
        else:
            bq[pl.ds(row, count), at : at + step] = value

    def subblock(source, j):
        return jnp.where(lax.rem(source, 2) == 0, j, n_split - 1 - j)

    def head_columns(d):
        return pl.ds(pl.multiple_of(d // n_split * VALUE_DIM, VALUE_DIM), VALUE_DIM)

    def send_kv(x, hf):
        for kind in range(2):
            for o in range(n):
                d = lax.rem(me + o, n)
                if hf is None:
                    src = akv.at[kind, x, :, :, :, head_columns(d)]
                    dst = kv.at[me, kind, x]
                else:
                    src = akv.at[kind, x, :, hf, :, head_columns(d)]
                    dst = kv.at[me, kind, x, :, hf]
                if o == 0:
                    pltpu.make_async_copy(src, dst, kv_recv.at[me]).start()
                else:
                    pltpu.make_async_remote_copy(
                        src_ref=src, dst_ref=dst, send_sem=kv_send.at[o], recv_sem=kv_recv.at[me],
                        device_id={"sp": d}, device_id_type=MESH,
                    ).start()

    def q_piece(d):
        start = pl.multiple_of(subblock(me, lax.rem(d, n_split)) * sub, sub)
        return aq.at[pl.ds(start, sub), head_columns(d)]

    def q_copy(o):
        d = lax.rem(me + o, n)
        return pltpu.make_async_remote_copy(
            src_ref=q_piece(d), dst_ref=qbuf.at[me], send_sem=q_send.at[o], recv_sem=q_recv.at[me],
            device_id={"sp": d}, device_id_type=MESH,
        )

    def near_copies():
        return [
            pltpu.make_async_remote_copy(
                src_ref=buf.at[pl.ds(rows, WINDOW)],
                dst_ref=buf.at[pl.ds(0, WINDOW)],
                send_sem=near_send.at[c],
                recv_sem=near_recv.at[c],
                device_id={"sp": lax.rem(me + 1, n)},
                device_id_type=MESH,
            )
            for c, buf in enumerate((kext, vext))
        ]

    @pl.loop(0, 2)
    def _(step):
        c_of = jnp.where(step == 0, core, 1 - core)
        row = pl.multiple_of((2 * chip + c_of) * part, part)

        @pl.when(step == 1)
        def _():
            own_copy(1 - core).wait_recv()

        def put(c, at, w, value):
            if c < 2:
                akv[c, chip, c_of, :, :, at : at + w] = value.reshape(2, half, w)
            else:
                put_rows(c, at, w, row, value)

        project_rows(lambda: xown[c_of], put, first=step == 0)

    send_kv(chip, None)

    for o in range(1, chips):
        x = lax.rem(chip + chips - o, chips)

        @pl.loop(0, 2)
        def _(hf):
            g_copy(o, hf).wait_recv()
            f_copy(o, hf, core).start()
            f_copy(o, hf, 1 - core).wait_recv()

            def put(c, at, w, value):
                value = value.reshape(2, half, w)
                for k in range(2):
                    if c < 2:
                        akv[c, x, k, hf, :, at : at + w] = value[k]
                    else:
                        row = pl.multiple_of((2 * x + k) * part + hf * half, half)
                        put_rows(c, at, w, row, value[k])

            project_rows(lambda: xrem[o - 1, hf].reshape(part, model), put)

            if o == chips - 1:
                @pl.when((hf == 1) & (me < n - 1))
                def _():
                    for copy in near_copies():
                        copy.start()

            send_kv(x, hf)

    pltpu.make_async_copy(q_piece(me), qbuf.at[me], q_recv.at[me]).start()
    for o in range(1, n):
        q_copy(o).start()

    @pl.loop(0, n_chunks)
    def _(cc):
        for copy in weight_copies(cc):
            copy.start()

    @pl.when(me == 0)
    def _():
        kext[pl.ds(0, WINDOW)] = jnp.zeros((WINDOW, kext.shape[1]), BF16)
        vext[pl.ds(0, WINDOW)] = jnp.zeros((WINDOW, vext.shape[1]), BF16)

    kv_heads = kext.shape[1] // HEAD_DIM
    group = bq.shape[1] // kext.shape[1]
    blocks = rows // WINDOW
    q_iota = lax.broadcasted_iota(jnp.int32, (WINDOW, 2 * WINDOW), 0)
    k_iota = lax.broadcasted_iota(jnp.int32, (WINDOW, 2 * WINDOW), 1)

    @pl.loop(0, blocks)
    def _(step):
        b = lax.rem(step + 1, blocks)

        @pl.when((b == 0) & (me > 0))
        def _():
            for copy in near_copies():
                copy.wait_recv()

        base = pl.multiple_of(b * WINDOW, WINDOW)
        first = (b == 0) & (me == 0)
        distance = q_iota + WINDOW - k_iota
        low = jnp.where(first, WINDOW, 0)
        allowed = (distance >= 0) & (distance < WINDOW) & (k_iota >= low)
        queries = bq[pl.ds(base, WINDOW), :].astype(F32) * HEAD_DIM ** (-0.5)
        queries = queries.astype(BF16)
        keys = kext[pl.ds(base, 2 * WINDOW), :]
        values = vext[pl.ds(base, 2 * WINDOW), :]
        for g in range(kv_heads):
            key = keys[:, g * HEAD_DIM : (g + 1) * HEAD_DIM]
            value = values[:, g * HEAD_DIM : (g + 1) * HEAD_DIM]
            for two in range(group // 2):
                both = []
                for e in range(2):
                    h = g * group + two * 2 + e
                    s = mm_t(queries[:, h * HEAD_DIM : (h + 1) * HEAD_DIM], key)
                    s = jnp.where(allowed, s, mask_fill)
                    top = jnp.maximum(jnp.max(s, axis=-1, keepdims=True), sink[h])
                    p = jnp.exp(s - top)
                    total = jnp.sum(p, axis=-1, keepdims=True) + jnp.exp(sink[h] - top)
                    both.append(mm((p * (1.0 / total)).astype(BF16), value).astype(BF16))
                at = (g * group + two * 2) * HEAD_DIM
                b_heads[pl.ds(base, WINDOW), at : at + 2 * HEAD_DIM] = jnp.concatenate(both, axis=1)

    my_head = me // n_split
    my_part = lax.rem(me, n_split)
    lane = lax.broadcasted_iota(jnp.int32, (sub, VALUE_DIM), 1)

    def ret_copy(i):
        row = pl.ds(pl.multiple_of(subblock(i, my_part) * sub, sub), sub)
        return pltpu.make_async_remote_copy(
            src_ref=obuf.at[i],
            dst_ref=hbuf.at[row, head_columns(me)],
            send_sem=ret_send.at[i],
            recv_sem=ret_recv.at[me],
            device_id={"sp": i},
            device_id_type=MESH,
        )

    def ret_local(i):
        row = pl.ds(pl.multiple_of(subblock(i, my_part) * sub, sub), sub)
        return pltpu.make_async_copy(obuf.at[i], hbuf.at[row, head_columns(me)], ret_recv.at[me])

    @pl.loop(0, n)
    def _(i):
        pltpu.make_async_copy(kv.at[i], kv.at[i], kv_recv.at[i]).wait()
        pltpu.make_async_copy(qbuf.at[i], qbuf.at[i], q_recv.at[i]).wait()
        q = qbuf[i].astype(F32) * HEAD_DIM ** (-0.5)
        qs[0] = jnp.where(lane < HEAD_DIM, q, 0.0).astype(BF16)
        qs[1] = jnp.where(lane >= HEAD_DIM, q, 0.0).astype(BF16)
        m_s[...] = jnp.full(m_s.shape, mask_fill, F32)
        l_s[...] = jnp.zeros(l_s.shape, F32)
        acc_s[...] = jnp.zeros(acc_s.shape, F32)
        first_row = subblock(i, my_part) * sub

        def block(j, diagonal):
            k = kv[j, 0].reshape(rows, VALUE_DIM)
            v = kv[j, 1].reshape(rows, VALUE_DIM)
            both = [mm_t(qs[m], k) for m in range(2)]
            for m, s in enumerate(both):
                if diagonal:
                    qpos = first_row + lax.broadcasted_iota(jnp.int32, s.shape, 0)
                    s = jnp.where(lax.broadcasted_iota(jnp.int32, s.shape, 1) <= qpos, s, mask_fill)
                old = m_s[m]
                new = jnp.maximum(old, jnp.max(s, axis=-1, keepdims=True))
                shrink = jnp.exp(old - new)
                p = jnp.exp(s - new[:, :1])
                folded = p[:, :VALUE_DIM]
                for c in range(1, s.shape[1] // VALUE_DIM):
                    folded = folded + p[:, c * VALUE_DIM : (c + 1) * VALUE_DIM]
                m_s[m] = new
                l_s[m] = l_s[m] * shrink + folded
                acc_s[m] = acc_s[m] * shrink + mm(p.astype(BF16), v)

        @pl.loop(0, i)
        def _(j):
            block(j, False)

        block(i, True)
        mean = [acc_s[m] / jnp.sum(l_s[m], axis=-1, keepdims=True) for m in range(2)]
        diff = mean[0] - lam[my_head] * mean[1]
        square = jnp.mean(diff * diff, axis=-1, keepdims=True)
        obuf[i] = (diff * lax.rsqrt(square + norm_eps) * gain[...] * head_scale).astype(BF16)

        @pl.when(i == me)
        def _():
            ret_local(i).start()

        @pl.when(i != me)
        def _():
            ret_copy(i).start()

    @pl.loop(0, n)
    def _(d):
        row = pl.ds(pl.multiple_of(subblock(me, lax.rem(d, n_split)) * sub, sub), sub)
        place = hbuf.at[row, head_columns(d)]
        pltpu.make_async_copy(place, place, ret_recv.at[d]).wait()

    def project(row, cc):
        return mm(b_heads[pl.ds(row, part), :], wb[cc]) + mm(hbuf[pl.ds(row, part), :], wa[cc])

    def row_of(x, c):
        return pl.multiple_of((2 * x + c) * part, part)

    def d_copy(cc):
        return pltpu.make_async_remote_copy(
            src_ref=dsend.at[cc], dst_ref=dbuf.at[cc],
            send_sem=d_send.at[cc], recv_sem=d_recv.at[cc],
            device_id={"tp": pair}, device_id_type=MESH,
        )

    def x_copy(cc, o):
        to = lax.rem(chip + o, chips)
        return pltpu.make_async_remote_copy(
            src_ref=xsend.at[cc, o - 1], dst_ref=xbuf.at[cc, o - 1],
            send_sem=x_send.at[cc, o - 1], recv_sem=x_recv.at[cc, o - 1],
            device_id={"tp": 2 * to + core}, device_id_type=MESH,
        )

    def pass_on(cc):
        d_copy(cc).wait_recv()
        for o in range(1, chips):
            xsend[cc, o - 1] = (own[cc, o] + dbuf[cc, o].astype(F32)).astype(BF16)
            x_copy(cc, o).start()

    @pl.loop(0, n_chunks)
    def _(cc):
        for copy in weight_copies(cc):
            copy.wait()
        for o in range(chips):
            dsend[cc, o] = project(row_of(lax.rem(chip + o, chips), 1 - core), cc).astype(BF16)
        d_copy(cc).start()
        for o in range(chips):
            own[cc, o] = project(row_of(lax.rem(chip + o, chips), core), cc)

        @pl.when(cc > 0)
        def _():
            pass_on(cc - 1)

    pass_on(n_chunks - 1)

    @pl.loop(0, n_chunks)
    def _(cc):
        total = own[cc, 0] + dbuf[cc, 0].astype(F32)
        for o in range(1, chips):
            x_copy(cc, o).wait_recv()
            total = total + xbuf[cc, o - 1].astype(F32)
        out[:, pl.ds(pl.multiple_of(cc * width, width), width)] = total.astype(BF16)

    @pl.when(me < n - 1)
    def _():
        for copy in near_copies():
            copy.wait_send()

    @pl.loop(1, n)
    def _(o):
        pltpu.make_async_copy(kv.at[0], kv.at[0], kv_send.at[o]).wait()
        q_copy(o).wait_send()

    own_copy(core).wait_send()
    for o in range(1, chips):
        for hf in range(2):
            g_copy(o, hf).wait_send()
            f_copy(o, hf, core).wait_send()

    @pl.loop(0, n)
    def _(i):
        @pl.when(i != me)
        def _():
            ret_copy(i).wait_send()

    @pl.loop(0, n_chunks)
    def _(cc):
        d_copy(cc).wait_send()
        for o in range(1, chips):
            x_copy(cc, o).wait_send()


def attend(n, n_tp, lam, sink, gain, inputs, wq, wk, wv, bwq, bwk, bwv, wa, wb):
    part, model = inputs.shape
    rows = part * n_tp
    half = part // 2
    local_heads = lam.shape[0]
    n_split = n // local_heads
    sub = rows // n_split
    width = 512
    n_chunks = model // width
    chips = n_tp // 2
    vm = pl.BlockSpec(memory_space=pltpu.VMEM)
    sm = pl.BlockSpec(memory_space=pltpu.SMEM)
    hbm = pl.BlockSpec(memory_space=pl.ANY)
    dma = pltpu.SemaphoreType.DMA
    return pl.pallas_call(
        functools.partial(attend_kernel, n, n_tp, n_split),
        out_shape=jax.ShapeDtypeStruct((part, model), BF16),
        in_specs=[sm, sm, vm] + [hbm] * 9,
        out_specs=vm,
        scratch_shapes=[
            pltpu.VMEM((2, part, model), BF16),
            pltpu.VMEM((chips - 1, 2, 2, half, model), BF16),
            pltpu.VMEM(wq.shape, BF16),
            pltpu.VMEM(wk.shape, BF16),
            pltpu.VMEM(wv.shape, BF16),
            pltpu.VMEM(bwq.shape, BF16),
            pltpu.VMEM(bwk.shape, BF16),
            pltpu.VMEM(bwv.shape, BF16),
            pltpu.VMEM((rows, wq.shape[1]), BF16),
            pltpu.VMEM((2, chips, 2, 2, half, wk.shape[1]), BF16),
            pltpu.VMEM((rows, bwq.shape[1]), BF16),
            pltpu.VMEM((n, 2, chips, 2, 2, half, VALUE_DIM), BF16),
            pltpu.VMEM((n, sub, VALUE_DIM), BF16),
            pltpu.VMEM((WINDOW + rows, bwk.shape[1]), BF16),
            pltpu.VMEM((WINDOW + rows, bwv.shape[1]), BF16),
            pltpu.VMEM((rows, local_heads * VALUE_DIM), BF16),
            pltpu.VMEM((n, sub, VALUE_DIM), BF16),
            pltpu.VMEM((2, sub, VALUE_DIM), BF16),
            pltpu.VMEM((2, sub, VALUE_DIM), F32),
            pltpu.VMEM((2, sub, VALUE_DIM), F32),
            pltpu.VMEM((2, sub, VALUE_DIM), F32),
            pltpu.VMEM((rows, bwq.shape[1]), BF16),
            pltpu.VMEM((n_chunks, wa.shape[0], width), BF16),
            pltpu.VMEM((n_chunks, wb.shape[0], width), BF16),
            pltpu.VMEM((n_chunks, chips, part, width), BF16),
            pltpu.VMEM((n_chunks, chips, part, width), BF16),
            pltpu.VMEM((n_chunks, chips, part, width), F32),
            pltpu.VMEM((n_chunks, chips - 1, part, width), BF16),
            pltpu.VMEM((n_chunks, chips - 1, part, width), BF16),
            dma,
            dma((6,)),
            dma((chips - 1, 2)),
            dma((chips - 1, 2)),
            dma((chips - 1, 2)),
            dma((chips - 1, 2)),
            dma,
            dma,
            dma((n,)),
            dma((n,)),
            dma((n,)),
            dma((n,)),
            dma((n,)),
            dma((n,)),
            dma((2,)),
            dma((2,)),
            dma((n_chunks, 2)),
            dma((n_chunks,)),
            dma((n_chunks,)),
            dma((n_chunks, chips - 1)),
            dma((n_chunks, chips - 1)),
        ],
        compiler_params=pltpu.CompilerParams(
            collective_id=0, has_side_effects=True, vmem_limit_bytes=63 * 1024 * 1024
        ),
    )(lam, sink, gain, inputs, wq, wk, wv, bwq, bwk, bwv, wa, wb)


def solution(mesh):
    n, n_tp = mesh.shape["sp"], mesh.shape["tp"]

    def shards(
        inputs, a_query_w, a_key_w, a_value_w, b_query_w, b_key_w, b_value_w,
        head_lambda, head_gain, sink_logit, a_out_w, b_out_w,
    ):
        return attend(
            n, n_tp, head_lambda, sink_logit, head_gain.reshape(1, VALUE_DIM), inputs,
            a_query_w, a_key_w, a_value_w, b_query_w, b_key_w, b_value_w, a_out_w, b_out_w,
        )

    return jax.shard_map(
        shards,
        mesh=mesh,
        in_specs=(
            P(("sp", "tp"), None),
            P(None, "tp"),
            P(None, "tp"),
            P(None, "tp"),
            P(None, "tp"),
            P(None, "tp"),
            P(None, "tp"),
            P("tp"),
            P(),
            P("tp"),
            P("tp", None),
            P("tp", None),
        ),
        out_specs=P(("sp", "tp"), None),
        check_vma=False,
    )
```
